32 devices in a mesh: rep: 2 (over x), fs: 8 (over z, y), tp: 2 (over core).
Axes of the slice: x: 2, y: 2, z: 4, core: 2. Of those that a mesh axis runs over, the one named last changes fastest.
Arguments:
- block_input: bfloat16 [8192, 2048], P(('rep', 'fs', 'tp')), may hold values from -6 to 6
- pre_gain: float32 [2048], replicated, may hold values from 0.1 to 1.9
- post_gain: float32 [2048], replicated, may hold values from 0.1 to 1.9
- gate_saved: bfloat16 [8192, 5632], P(('rep', 'fs'), 'tp'), may hold values from -8 to 8
- up_saved: bfloat16 [8192, 5632], P(('rep', 'fs'), 'tp'), may hold values from -6 to 6
- branch_saved: bfloat16 [8192, 2048], P(('rep', 'fs', 'tp')), may hold values from -6 to 6
- out_cotangent: bfloat16 [8192, 2048], P(('rep', 'fs', 'tp')), may hold values from -6 to 6
- gate_weight: bfloat16 [2048, 5632], P('fs', 'tp'), may hold values from -0.125 to 0.125
- up_weight: bfloat16 [2048, 5632], P('fs', 'tp'), may hold values from -0.125 to 0.125
- down_weight: bfloat16 [2048, 5632], P('fs', 'tp'), may hold values from -0.078125 to 0.078125
Outputs:
- input_grad: bfloat16 [8192, 2048], P(('rep', 'fs', 'tp'))
- gate_grad: float32 [2048, 5632], P('fs', 'tp')
- up_grad: float32 [2048, 5632], P('fs', 'tp')
- down_grad: float32 [2048, 5632], P('fs', 'tp')
The draws below stay inside these ranges and needn't reach their ends.
All inputs are finite; a program needn't handle non-finite values.
Results may differ from the reference program's by a relative error of at most 0.018.
Values may be sent and summed in bfloat16 or wider, within the bound.
A program may use at most 128 MiB of HBM per device.

```python
import jax
import jax.numpy as jnp
from jax import lax

D = 2048
FF = 5632
TOKENS = 8192
N_TP = 2


def spiked(array, key, source, target, shards_of, factor):
    owner, partner = [(jnp.arange(array.shape[position]) // (array.shape[position] // shards_of)).reshape([-1 if axis == position else 1 for axis in range(array.ndim)]) for position in (source, target)]
    chosen = jax.random.permutation(key, shards_of)[partner]
    strong = (owner == chosen) | (owner == (partner + shards_of // 2) % shards_of)
    return jnp.where(strong, factor * array, array)


def shard_levels(key, dims, cuts, least, high):
    def one(position, parts):
        draws = jax.random.uniform(jax.random.fold_in(jax.random.fold_in(key, 6), position), (parts,), jnp.float32, least / len(cuts), high / len(cuts))
        return jnp.repeat(jnp.exp(draws), dims[position] // parts).reshape((-1,) + (1,) * (len(dims) - position - 1))

    factor_of = one(*cuts[0])
    for cut in cuts[1:]:
        factor_of = factor_of * one(*cut)
    return factor_of


def centred(key, shape, deviation, reach, pieces=(), dtype=jnp.bfloat16):
    factor_of = shard_levels(key, shape, pieces, -0.22, 0.18) if pieces else 1.0
    values = jax.random.normal(key, shape, jnp.float32) * deviation * factor_of
    return jnp.minimum(jnp.maximum(values, -reach), reach).astype(dtype)


def bell_draw_with(stream_key, dims, deviation, bound, pieces, heavy, dtype=jnp.bfloat16):
    drawn = deviation * jax.random.normal(stream_key, dims, jnp.float32)
    if pieces:
        drawn = drawn * shard_levels(stream_key, dims, pieces, -0.22, 0.18)
    return jnp.clip(spiked(drawn, jax.random.fold_in(stream_key, 3), *heavy), -bound, bound).astype(dtype)


def setup_inputs(seed: int = 0) -> dict:
    streams_of = jax.random.split(jax.random.key(seed), 11)
    return {
        "block_input": centred(streams_of[0], (TOKENS, D), 1.0, 6.0, ((0, 32),)),
        "pre_gain": jnp.clip(1.0 + 0.18 * jax.random.normal(streams_of[1], (D,), jnp.float32), 0.1, 1.9),
        "post_gain": jnp.clip(1.0 + 0.18 * jax.random.normal(streams_of[2], (D,), jnp.float32), 0.1, 1.9),
        "gate_saved": centred(streams_of[3], (TOKENS, FF), 1.5, 8.0, ((0, 16), (1, 2))),
        "up_saved": centred(streams_of[4], (TOKENS, FF), 1.0, 6.0, ((0, 16), (1, 2))),
        "branch_saved": centred(streams_of[5], (TOKENS, D), 1.0, 6.0, ((0, 32),)),
        "out_cotangent": bell_draw_with(streams_of[6], (TOKENS, D), 1.0, 6.0, ((0, 32),), (0, 1, 32, 2.75)),
        "gate_weight": centred(streams_of[7], (D, FF), D ** -0.5, 0.125, ((0, 8), (1, 2))),
        "up_weight": centred(streams_of[8], (D, FF), D ** -0.5, 0.125, ((0, 8), (1, 2))),
        "down_weight": centred(streams_of[9], (D, FF), FF ** -0.5, 0.078125, ((0, 8), (1, 2))),
    }


eps = 1e-06

def contract_rows(left, right):
    return lax.dot_general(left, right, (((0,), (0,)), ((), ())), preferred_element_type=jnp.float32)

def contract_cols(left, right):
    return lax.dot_general(left, right, (((1,), (1,)), ((), ())), preferred_element_type=jnp.float32)

def reference(block_input, pre_gain, post_gain, gate_saved, up_saved, branch_saved, out_cotangent, gate_weight, up_weight, down_weight):
    xfull = block_input.astype(jnp.float32)
    inv_x = lax.rsqrt(lax.optimization_barrier(jnp.mean(xfull * xfull, axis=-1, keepdims=True)) + eps)
    normed = (xfull * inv_x * pre_gain).astype(jnp.bfloat16)
    branch = branch_saved.astype(jnp.float32)
    inv_b = lax.rsqrt(lax.optimization_barrier(jnp.mean(branch * branch, axis=-1, keepdims=True)) + eps)
    upstream = 0.5 * out_cotangent.astype(jnp.float32) * post_gain
    branch_grad = (inv_b * upstream - branch * inv_b ** 3 * lax.optimization_barrier(jnp.mean(upstream * branch, axis=-1, keepdims=True))).astype(jnp.bfloat16)
    gate_f = gate_saved.astype(jnp.float32)
    up_f = up_saved.astype(jnp.float32)
    sigma = jax.nn.sigmoid(gate_f)
    silu_gate = gate_f * sigma
    hidden = (silu_gate * up_f).astype(jnp.bfloat16)
    hidden_grad = jnp.dot(branch_grad, down_weight, preferred_element_type=jnp.float32)
    gate_cot = (hidden_grad * up_f * sigma * (1.0 + gate_f * (1.0 - sigma))).astype(jnp.bfloat16)
    up_cot = (hidden_grad * silu_gate).astype(jnp.bfloat16)
    width = FF // N_TP
    normed_grad = jnp.zeros(xfull.shape, jnp.float32)
    for group in range(N_TP):
        lo = group * width
        partial_sum = contract_cols(gate_cot[:, lo:lo + width], gate_weight[:, lo:lo + width])
        partial_sum = partial_sum + contract_cols(up_cot[:, lo:lo + width], up_weight[:, lo:lo + width])
        normed_grad = normed_grad + lax.optimization_barrier(partial_sum.astype(jnp.bfloat16)).astype(jnp.float32)
    scaled = normed_grad * pre_gain
    input_grad = out_cotangent.astype(jnp.float32) + inv_x * scaled - xfull * inv_x ** 3 * lax.optimization_barrier(jnp.mean(scaled * xfull, axis=-1, keepdims=True))
    gate_grad = contract_rows(normed, gate_cot)
    up_grad = contract_rows(normed, up_cot)
    down_grad = contract_rows(branch_grad, hidden)
    return (input_grad.astype(jnp.bfloat16), gate_grad, up_grad, down_grad)
```

```python
import functools

import jax
import jax.numpy as jnp
from jax import lax
from jax.sharding import PartitionSpec as P

eps = 1e-06


def contract_rows(left, right):
    return lax.dot_general(
        left, right, (((0,), (0,)), ((), ())), preferred_element_type=jnp.float32
    )


def contract_cols(left, right):
    return lax.dot_general(
        left, right, (((1,), (1,)), ((), ())), preferred_element_type=jnp.float32
    )


def shifted(value, reps, step):
    return lax.ppermute(value, "rep", [(i, (i + step) % reps) for i in range(reps)])


def per_device(
    reps,
    block_input,
    pre_gain,
    post_gain,
    gate_saved,
    up_saved,
    branch_saved,
    out_cotangent,
    gate_weight,
    up_weight,
    down_weight,
):
    bf16, f32 = jnp.bfloat16, jnp.float32
    me = lax.axis_index("rep")
    width = gate_saved.shape[1] // reps

    def columns(value, owner):
        return lax.dynamic_slice_in_dim(value, owner * width, width, axis=1)

    down_full = lax.all_gather(columns(down_weight, me), "fs", axis=0, tiled=True)

    gates = [columns(gate_saved, me)]
    ups = [columns(up_saved, me)]
    for k in range(1, reps):
        there = lax.rem(me + k, reps)
        gates.append(shifted(columns(gate_saved, there), reps, k))
        ups.append(shifted(columns(up_saved, there), reps, k))

    xfull = block_input.astype(f32)
    inv_x = lax.rsqrt(jnp.mean(xfull * xfull, axis=-1, keepdims=True) + eps)
    normed = (xfull * inv_x * pre_gain).astype(bf16)
    branch = branch_saved.astype(f32)
    inv_b = lax.rsqrt(jnp.mean(branch * branch, axis=-1, keepdims=True) + eps)
    upstream = 0.5 * out_cotangent.astype(f32) * post_gain
    branch_grad = (
        inv_b * upstream - branch * inv_b**3 * jnp.mean(upstream * branch, axis=-1, keepdims=True)
    ).astype(bf16)

    normed_own = [normed] + [shifted(normed, reps, k) for k in range(1, reps)]
    branch_own = [branch_grad] + [shifted(branch_grad, reps, k) for k in range(1, reps)]
    normed_rows = [lax.all_gather(v, "tp", axis=0, tiled=True) for v in normed_own]
    branch_rows = [lax.all_gather(v, "tp", axis=0, tiled=True) for v in branch_own]
    normed_all = jnp.concatenate(normed_rows, axis=0)
    branch_all = jnp.concatenate(branch_rows, axis=0)

    gate_f = jnp.concatenate(gates, axis=0).astype(f32)
    up_f = jnp.concatenate(ups, axis=0).astype(f32)
    sigma = jax.nn.sigmoid(gate_f)
    silu_gate = gate_f * sigma
    hidden = (silu_gate * up_f).astype(bf16)

    def spread(total):
        shard = lax.psum_scatter(total.astype(bf16), "fs", scatter_dimension=0, tiled=True)
        out = jnp.zeros((shard.shape[0], width * reps), f32)
        out = lax.dynamic_update_slice_in_dim(out, shard.astype(f32), me * width, axis=1)
        for k in range(1, reps):
            other = shifted(shard, reps, k).astype(f32)
            out = lax.dynamic_update_slice_in_dim(
                out, other, lax.rem(me - k + reps, reps) * width, axis=1
            )
        return out

    down_grad = spread(contract_rows(branch_all, hidden))

    hidden_grad = jnp.dot(branch_all, down_full, preferred_element_type=f32)
    gate_cot = (hidden_grad * up_f * sigma * (1.0 + gate_f * (1.0 - sigma))).astype(bf16)
    up_cot = (hidden_grad * silu_gate).astype(bf16)
    gate_grad = spread(contract_rows(normed_all, gate_cot))
    up_grad = spread(contract_rows(normed_all, up_cot))

    gate_full = lax.all_gather(columns(gate_weight, me), "fs", axis=0, tiled=True)
    up_full = lax.all_gather(columns(up_weight, me), "fs", axis=0, tiled=True)
    partial = (contract_cols(gate_cot, gate_full) + contract_cols(up_cot, up_full)).astype(bf16)
    rows = partial.shape[0] // reps
    normed_grad = None
    for k in range(reps):
        piece = lax.psum_scatter(
            partial[k * rows : (k + 1) * rows], "tp", scatter_dimension=0, tiled=True
        )
        if k:
            piece = shifted(piece, reps, reps - k)
        piece = piece.astype(f32)
        normed_grad = piece if normed_grad is None else normed_grad + piece

    scaled = normed_grad * pre_gain
    input_grad = (
        out_cotangent.astype(f32)
        + inv_x * scaled
        - xfull * inv_x**3 * jnp.mean(scaled * xfull, axis=-1, keepdims=True)
    )
    return (input_grad.astype(bf16), gate_grad, up_grad, down_grad)


def solution(mesh):
    return jax.shard_map(
        functools.partial(per_device, mesh.shape["rep"]),
        mesh=mesh,
        in_specs=(
            P(("rep", "fs", "tp"), None),
            P(),
            P(),
            P(("rep", "fs"), "tp"),
            P(("rep", "fs"), "tp"),
            P(("rep", "fs", "tp"), None),
            P(("rep", "fs", "tp"), None),
            P("fs", "tp"),
            P("fs", "tp"),
            P("fs", "tp"),
        ),
        out_specs=(P(("rep", "fs", "tp"), None), P("fs", "tp"), P("fs", "tp"), P("fs", "tp")),
        check_vma=False,
    )
```
